32 devices in a mesh: sp: 8 (over z, y), tp: 4 (over x, core).
Axes of the slice: x: 2, y: 2, z: 4, core: 2. Of those that a mesh axis runs over, the one named last changes fastest.
Arguments:
- d_out: bfloat16 [4096, 2048], P('sp'), may hold values from -6 to 6
- route_expert: int32 [4096, 2], P('sp'), may hold values from 0 to 7, all different within a row; in each aligned block of 512 rows (0 to 511, 512 to 1023, ...) at most 144 rows name the same one
- route_weight: float32 [4096, 2], P('sp'), may hold values from 0.2 to 1
- expert_inputs: bfloat16 [8, 1152, 2048], P('sp'), may hold values from -6 to 6
- w_gate: bfloat16 [8, 2048, 2816], P('sp', None, 'tp'), may hold values from -0.125 to 0.125
- w_up: bfloat16 [8, 2048, 2816], P('sp', None, 'tp'), may hold values from -0.125 to 0.125
- w_down: bfloat16 [8, 2816, 2048], P('sp', 'tp'), may hold values from -0.109375 to 0.109375
- w_out: bfloat16 [2048, 1024], P(None, 'tp'), may hold values from -0.1875 to 0.1875
- queries: bfloat16 [4096, 4, 128], P('sp', 'tp'), may hold values from -6 to 6
- keys: bfloat16 [4096, 4, 128], P('sp', 'tp'), may hold values from -2 to 2
- values: bfloat16 [4096, 4, 256], P('sp', 'tp'), may hold values from -6 to 6
- log_decay: float32 [4096, 4, 128], P('sp', 'tp'), may hold values from -1 to 0
Outputs:
- grad_gate: bfloat16 [8, 2048, 2816], P('sp', None, 'tp')
- grad_up: bfloat16 [8, 2048, 2816], P('sp', None, 'tp')
- grad_down: bfloat16 [8, 2816, 2048], P('sp', 'tp')
- grad_proj: float32 [2048, 1024], P('sp', 'tp')
- grad_queries: bfloat16 [4096, 4, 128], P('sp', 'tp')
- grad_keys: bfloat16 [4096, 4, 128], P('sp', 'tp')
- grad_values: bfloat16 [4096, 4, 256], P('sp', 'tp')
- grad_log_decay: float32 [4096, 4, 128], P('sp', 'tp')
The draws below stay inside these ranges and needn't reach their ends.
Inputs may be any that keep to these rules, and one draw needn't show every extreme that they name: `route_expert`: the two experts of a token differ. Among the rows of one device no expert is named more than 144 times, and in every draw some device names some expert exactly 144 times.
All inputs are finite; a program needn't handle non-finite values.
Results may differ from the reference program's by a relative error of at most 0.02.
Values may be sent and summed in bfloat16 or wider, within the bound.
A program may use at most 128 MiB of HBM per device.

```python
import math
import jax
import jax.numpy as jnp
import numpy as np
from jax import lax

D = 2048
FF = 2816
MIXER_HEADS = 4
KEY_CHANNELS = 128
DV = 256
BLK = 64
TOK_DEV = 512
SEQUENCE_TOKENS = 4096
EXPERTS = 8
CAP = 144
N_SP = 8
N_TP = 4


def draw_log_decay(key, part):
    every_head_keys = jax.random.split(jax.random.fold_in(key, 11), 7)
    slow_share = 0.5
    gradual_decay_mask = jax.random.bernoulli(every_head_keys[0], slow_share, (MIXER_HEADS, KEY_CHANNELS))
    slow_rate = jnp.exp(jax.random.uniform(every_head_keys[1], (MIXER_HEADS, KEY_CHANNELS), jnp.float32, jnp.log(0.05), jnp.log(0.5))) / SEQUENCE_TOKENS
    fast_rate = jnp.exp(jax.random.uniform(every_head_keys[2], (MIXER_HEADS, KEY_CHANNELS), jnp.float32, jnp.log(0.01), jnp.log(0.033)))
    base_rate = jnp.where(gradual_decay_mask, slow_rate, fast_rate)
    segment_count = SEQUENCE_TOKENS // TOK_DEV
    device_factor = jnp.exp(jax.random.uniform(every_head_keys[3], (segment_count, 1, 1, 1), jnp.float32, jnp.log(0.5), jnp.log(2.0)))
    device_factor = jnp.broadcast_to(device_factor, (segment_count, TOK_DEV, 1, 1)).reshape(SEQUENCE_TOKENS, 1, 1)
    roughness = jax.random.uniform(every_head_keys[4], (SEQUENCE_TOKENS, MIXER_HEADS, KEY_CHANNELS), jnp.float32, 0.5, 1.5)
    spike_position = jax.random.randint(every_head_keys[5], (4,), 0, SEQUENCE_TOKENS)
    spike_token_rows = jnp.any(jnp.arange(SEQUENCE_TOKENS)[:, None] == spike_position[None, :], axis=1)
    spike_penalty = jnp.log(jax.random.uniform(every_head_keys[6], (SEQUENCE_TOKENS, MIXER_HEADS, KEY_CHANNELS), jnp.float32, 0.5, 0.8))
    channel_decay_logs = -base_rate[None] * device_factor * roughness
    channel_decay_logs = channel_decay_logs + jnp.where(spike_token_rows[:, None, None] & gradual_decay_mask[None], spike_penalty, 0.0)
    return channel_decay_logs.astype(jnp.float32)


def with_spikes(drawn, own_key, source, target, shards_of, factor):
    def block_of(position):
        return (jnp.arange(drawn.shape[position]) // (drawn.shape[position] // shards_of)).reshape((-1,) + (1,) * (drawn.ndim - 1 - position))

    near = jax.random.permutation(own_key, shards_of)[block_of(target)]
    far = (block_of(target) + shards_of // 2) % shards_of
    return jnp.where((block_of(source) == near) | (block_of(source) == far), factor * drawn, drawn)


def levels(rng, dims, shards, least, largest):
    loudness = 1.0
    for dim, shards_of in shards:
        steps = jax.random.uniform(jax.random.fold_in(jax.random.fold_in(rng, 6), dim), (shards_of,), jnp.float32, least / len(shards), largest / len(shards))
        loudness = loudness * jnp.repeat(jnp.exp(steps), dims[dim] // shards_of).reshape((-1,) + (1,) * (len(dims) - 1 - dim))
    return loudness


def assign_block(own_key, own, number, rows, amount, top, reach, skew):
    ranking = jax.random.permutation(own_key, amount)
    crowded, ordinary = load_shares(amount, rows * top, reach, skew, True), load_shares(amount, rows * top, reach, skew, False)
    places = jnp.arange(amount)

    def named(sizes, turn):
        used = int((sizes > 0).sum())
        fixed = max(1, used // 4)
        passed = fixed + (places - fixed + turn * (used - fixed)) % max(1, amount - fixed)
        return jnp.zeros((amount,), jnp.int32).at[ranking[jnp.where(places < fixed, places, passed)]].set(jnp.asarray(sizes, jnp.int32))

    sizes = jnp.where(number % 4 == 0, named(crowded, number // 4), named(ordinary, number - number // 4 - 1))
    mixed = jax.random.permutation(jax.random.fold_in(own, 3), amount)
    giver, receiver = mixed[0:amount // 2 * 2:2], mixed[1:amount // 2 * 2:2]
    slack = jnp.minimum(sizes[giver] - 1, reach - sizes[receiver]) // 2
    slack = jnp.where((giver == ranking[0]) | (receiver == ranking[0]) | (sizes[receiver] == 0), 0, jnp.maximum(slack, 0))
    passed = jax.random.randint(jax.random.fold_in(own, 4), (amount // 2,), 0, 1 << 20) % (slack + 1)
    sizes = sizes.at[giver].add(-passed).at[receiver].add(passed)
    members = jnp.searchsorted(jnp.cumsum(sizes), jnp.arange(rows * top), side="right").astype(jnp.int32)
    grid = members.reshape(top, rows).T
    grid = grid[jax.random.permutation(jax.random.fold_in(own, 1), rows)]
    turn = jax.random.randint(jax.random.fold_in(own, 2), (rows, 1), 0, top)
    return jnp.take_along_axis(grid, (jnp.arange(top)[None, :] + turn) % top, axis=1)


def load_shares(amount, total, reach, lean, full):
    weights = [(1 << 20) // math.isqrt(grade ** lean) + 1 for grade in range(1, amount + 1)]
    largest = reach if full else min(reach, max(-(-total // amount), total * weights[0] // sum(weights)))
    least = 1 if total - largest >= amount - 1 else 0
    given, surplus = [largest] + [least] * (amount - 1), total - largest - least * (amount - 1)
    while surplus > 0:
        movable = [i for i in range(1, amount) if given[i] < largest] or [i for i in range(1, amount) if given[i] < reach]
        mass, budget = sum([weights[i] for i in movable]), surplus
        for i in movable:
            extra = min(reach - given[i], max(1, budget * weights[i] // mass), surplus)
            given[i] = given[i] + extra
            surplus = surplus - extra
    return np.array(given)


def gaussian(stream_key, shape, width, limit, shards=(), kind=jnp.bfloat16):
    loudness = levels(stream_key, shape, shards, -0.22, 0.18) if shards else 1.0
    entries = jax.random.normal(stream_key, shape, jnp.float32) * width * loudness
    return jnp.minimum(jnp.maximum(entries, -limit), limit).astype(kind)


def gaussian_with(rng, dims, scale, bound, cuts, heavy, kind=jnp.bfloat16):
    values = scale * jax.random.normal(rng, dims, jnp.float32)
    if cuts:
        values = values * levels(rng, dims, cuts, -0.22, 0.18)
    return jnp.clip(with_spikes(values, jax.random.fold_in(rng, 3), *heavy), -bound, bound).astype(kind)


def setup_inputs(seed: int = 0) -> dict:
    splits = jax.random.split(jax.random.key(seed), 13)
    d_out = gaussian_with(splits[0], (SEQUENCE_TOKENS, D), 1.0, 6.0, ((0, 8),), (0, 1, 8, 2.0))
    route_expert_keys = jax.random.split(jax.random.fold_in(splits[1], 1), SEQUENCE_TOKENS // TOK_DEV)
    route_expert_turns = jax.random.permutation(jax.random.fold_in(splits[1], 3), SEQUENCE_TOKENS // TOK_DEV)
    route_expert = jax.vmap(lambda own, number: assign_block(jax.random.fold_in(splits[1], 2), own, number, TOK_DEV, EXPERTS, 2, CAP, 0))(route_expert_keys, route_expert_turns).reshape((SEQUENCE_TOKENS, 2))
    route_weight = jnp.clip(0.2 + 0.8 * jax.random.uniform(splits[2], (SEQUENCE_TOKENS, 2), jnp.float32) ** levels(splits[2], (SEQUENCE_TOKENS, 2), ((0, 8),), -0.2, 0.2), 0.2, 1.0)
    expert_inputs = gaussian(splits[3], (EXPERTS, EXPERTS * CAP, D), 1.0, 6.0, ((0, 8),))
    w_gate = gaussian(splits[4], (EXPERTS, D, FF), D ** -0.5, 0.125, ((0, 8), (2, 4)))
    w_up = gaussian(splits[5], (EXPERTS, D, FF), D ** -0.5, 0.125, ((0, 8), (2, 4)))
    w_down = gaussian(splits[6], (EXPERTS, FF, D), FF ** -0.5, 0.109375, ((0, 8), (1, 4)))
    w_out = gaussian(splits[7], (D, MIXER_HEADS * DV), (MIXER_HEADS * DV) ** -0.5, 0.1875, ((1, 4),))
    queries = gaussian(splits[8], (SEQUENCE_TOKENS, MIXER_HEADS, KEY_CHANNELS), 1.0, 6.0, ((0, 8), (1, 4)))
    keys = gaussian(splits[9], (SEQUENCE_TOKENS, MIXER_HEADS, KEY_CHANNELS), (SEQUENCE_TOKENS ** -0.25), 2.0, ((0, 8), (1, 4)))
    values = gaussian(splits[10], (SEQUENCE_TOKENS, MIXER_HEADS, DV), 1.0, 6.0, ((0, 8), (1, 4)))
    log_decay = draw_log_decay(jax.random.fold_in(splits[12], 71), 0)
    return dict(d_out=d_out, route_expert=route_expert, route_weight=route_weight, expert_inputs=expert_inputs, w_gate=w_gate, w_up=w_up, w_down=w_down, w_out=w_out, queries=queries, keys=keys, values=values, log_decay=log_decay)


precise = lax.Precision.HIGHEST

def block_mixer(scaled_queries, keys_in, values_in, decay_in, initial):
    length, head_count, _ = scaled_queries.shape
    value_width = values_in.shape[-1]
    count_blocks = length // BLK

    def to_blocks(tensor):
        return tensor.reshape(count_blocks, BLK, head_count, tensor.shape[-1]).transpose(0, 2, 1, 3)
    causal = jnp.tril(jnp.ones((BLK, BLK), dtype=bool))[:, :, None]

    def advance(carry_state, inputs):
        query_block, key_block, value_block, decay_block = inputs
        cumulative = jnp.cumsum(decay_block, axis=1)
        ending = cumulative[:, -1, :]
        carried = jnp.einsum('hcd,hde->hce', query_block * jnp.exp(cumulative), carry_state, precision=precise)
        within = jnp.where(causal, jnp.exp(cumulative[:, :, None, :] - cumulative[:, None, :, :]), 0.0)
        scores = jnp.einsum('hid,hjd,hijd->hij', query_block, key_block, within, precision=precise)
        inner_part = jnp.einsum('hij,hje->hie', scores, value_block, precision=precise)
        faded_keys = key_block * jnp.exp(ending[:, None, :] - cumulative)
        carry_state = carry_state * jnp.exp(ending)[:, :, None] + jnp.einsum('hcd,hce->hde', faded_keys, value_block, precision=precise)
        return (carry_state, carried + inner_part)
    final_state, blocks_out = lax.scan(jax.checkpoint(advance), initial, (to_blocks(scaled_queries), to_blocks(keys_in), to_blocks(values_in), to_blocks(decay_in)))
    return (blocks_out.transpose(0, 2, 1, 3).reshape(length, head_count, value_width), final_state)

def expert_pass(rows_in, routed_rows, gate_w, up_w, down_w):
    gate_pre = jnp.dot(rows_in, gate_w, preferred_element_type=jnp.float32)
    up_pre = jnp.dot(rows_in, up_w, preferred_element_type=jnp.float32)
    sigmoid_gate = jax.nn.sigmoid(gate_pre)
    active = gate_pre * sigmoid_gate
    hidden = (active * up_pre).astype(jnp.bfloat16)
    d_hidden = lax.dot_general(routed_rows, down_w, (((1,), (1,)), ((), ())), preferred_element_type=jnp.float32)
    d_gate = (d_hidden * up_pre * sigmoid_gate * (1.0 + gate_pre * (1.0 - sigmoid_gate))).astype(jnp.bfloat16)
    d_up = (d_hidden * active).astype(jnp.bfloat16)
    rows_first = (((0,), (0,)), ((), ()))
    grad_gate = lax.dot_general(rows_in, d_gate, rows_first, preferred_element_type=jnp.float32).astype(jnp.bfloat16)
    grad_up = lax.dot_general(rows_in, d_up, rows_first, preferred_element_type=jnp.float32).astype(jnp.bfloat16)
    grad_down = lax.dot_general(hidden, routed_rows, rows_first, preferred_element_type=jnp.float32).astype(jnp.bfloat16)
    return (grad_gate, grad_up, grad_down, d_gate, d_up)

def reference(d_out, route_expert, route_weight, expert_inputs, w_gate, w_up, w_down, w_out, queries, keys, values, log_decay):
    per_block = route_expert.reshape(N_SP, 2 * TOK_DEV).astype(jnp.int32)
    onehot = (per_block[:, :, None] == jnp.arange(EXPERTS, dtype=jnp.int32)[None, None, :]).astype(jnp.int32)
    before = jnp.cumsum(onehot, axis=1) - onehot
    rank_slot = lax.optimization_barrier(jnp.sum(before * onehot, axis=2))
    source_dev = jnp.arange(N_SP, dtype=jnp.int32)[:, None]
    slot_index = (per_block * (N_SP * CAP) + source_dev * CAP + rank_slot).reshape(-1).astype(jnp.int32)
    scaled = (jnp.repeat(d_out, 2, axis=0).astype(jnp.float32) * route_weight.reshape(-1)[:, None]).astype(jnp.bfloat16)
    routed = jnp.zeros((EXPERTS * N_SP * CAP, D), jnp.bfloat16).at[slot_index].set(scaled).reshape(EXPERTS, N_SP * CAP, D)
    part_width = FF // N_TP

    def one_expert(operands):
        rows_in, routed_rows, gate_w, up_w, down_w = operands
        grad_gate, grad_up, grad_down, d_gate, d_up = expert_pass(rows_in, routed_rows, gate_w, up_w, down_w)
        total = jnp.zeros((rows_in.shape[0], D), jnp.float32)
        for piece in range(N_TP):
            lower = piece * part_width
            term = lax.dot_general(d_gate[:, lower:lower + part_width], gate_w[:, lower:lower + part_width], (((1,), (1,)), ((), ())), preferred_element_type=jnp.float32)
            term = term + lax.dot_general(d_up[:, lower:lower + part_width], up_w[:, lower:lower + part_width], (((1,), (1,)), ((), ())), preferred_element_type=jnp.float32)
            total = total + lax.optimization_barrier(term.astype(jnp.bfloat16)).astype(jnp.float32)
        return (grad_gate, grad_up, grad_down, total.astype(jnp.bfloat16))
    grad_gate, grad_up, grad_down, row_grads = lax.map(one_expert, (expert_inputs, routed, w_gate, w_up, w_down))
    picked = row_grads.reshape(-1, D)[slot_index].astype(jnp.float32).reshape(SEQUENCE_TOKENS, 2, D).sum(axis=1)
    mix_grad = (d_out.astype(jnp.float32) + picked).astype(jnp.bfloat16)
    scale_q = KEY_CHANNELS ** (-0.5)
    initial = jnp.zeros((MIXER_HEADS, KEY_CHANNELS, DV), jnp.float32)

    def mixer_map(query_x, key_x, value_x, decay_x):
        return block_mixer(query_x * scale_q, key_x, value_x, decay_x, initial)[0]
    mixer_out, pullback = jax.vjp(mixer_map, queries.astype(jnp.float32), keys.astype(jnp.float32), values.astype(jnp.float32), log_decay)
    mixed = mixer_out.reshape(SEQUENCE_TOKENS, MIXER_HEADS * DV).astype(jnp.bfloat16)
    grad_proj = lax.dot_general(mix_grad, mixed, (((0,), (0,)), ((), ())), preferred_element_type=jnp.float32)
    d_mixed = jnp.dot(mix_grad, w_out, preferred_element_type=jnp.float32).reshape(SEQUENCE_TOKENS, MIXER_HEADS, DV)
    grad_q, grad_k, grad_v, grad_g = pullback(d_mixed)
    return (grad_gate, grad_up, grad_down, grad_proj, grad_q.astype(jnp.bfloat16), grad_k.astype(jnp.bfloat16), grad_v.astype(jnp.bfloat16), grad_g)
```

```python
import functools

import jax
import jax.numpy as jnp
from jax import lax
from jax.experimental import pallas as pl
from jax.experimental.pallas import tpu as pltpu
from jax.sharding import PartitionSpec as P

BLK = 64


precise = lax.Precision.HIGHEST


MESH = pl.DeviceIdType.MESH
NN = (((1,), (0,)), ((), ()))
NT = (((1,), (1,)), ((), ()))
TN = (((0,), (0,)), ((), ()))


def mm(a, b, dims):
    return lax.dot_general(a, b, dims, preferred_element_type=jnp.float32)


def triangle(lower):
    rows = lax.broadcasted_iota(jnp.int32, (BLK, BLK), 0)
    cols = lax.broadcasted_iota(jnp.int32, (BLK, BLK), 1)
    return rows >= cols if lower else rows <= cols


def block_sums(mask, x):
    return lax.dot_general(
        mask.astype(jnp.float32), x, NN, precision=precise, preferred_element_type=jnp.float32
    )


def decays(g_ref, rows):
    cumulative = block_sums(triangle(True), g_ref[rows, :])
    middle = cumulative[BLK // 2 - 1 : BLK // 2, :]
    ending = cumulative[BLK - 1 : BLK, :]
    return cumulative, middle, ending


def greet(n, me):
    barrier = pltpu.get_barrier_semaphore()
    for k in range(1, n):
        pl.semaphore_signal(
            barrier, inc=1, device_id={"sp": lax.rem(me + k, n)}, device_id_type=MESH
        )
    return barrier


def state_copies(n, me, step, send_ref, recv_ref, send_sem, recv_sem):
    return [
        pltpu.make_async_remote_copy(
            src_ref=send_ref,
            dst_ref=recv_ref.at[k - 1],
            send_sem=send_sem.at[k - 1],
            recv_sem=recv_sem.at[k - 1],
            device_id={"sp": lax.rem(me + step * k + n, n)},
            device_id_type=MESH,
        )
        for k in range(1, n)
    ]


def collect(n, me, step, copies, recv_ref, total, width):
    total[...] = jnp.zeros_like(total)
    for k in range(n - 1, 0, -1):
        copies[k - 1].wait()
        source = me - step * k
        reached = jnp.logical_and(source >= 0, source < n)

        @pl.when(reached)
        def _():
            factor = recv_ref[k - 1, width : width + 1, :].astype(jnp.float32)
            total[...] = total[...] * factor + recv_ref[k - 1, :width, :].astype(jnp.float32)


def forward_kernel(
    n, scale, q_ref, k_ref, v_ref, g_ref, mixed_ref, states_ref, kept, total, send, recv, ssem, rsem
):
    me = lax.axis_index("sp")
    barrier = greet(n, me)
    length, width = v_ref.shape
    blocks = length // BLK
    causal = triangle(True)
    local = jnp.zeros(total.shape, jnp.float32)
    ahead = jnp.zeros((1, q_ref.shape[1]), jnp.float32)
    befores = []
    for b in range(blocks):
        rows = pl.ds(b * BLK, BLK)
        cumulative, _, ending = decays(g_ref, rows)
        kept[b] = local
        befores.append(ahead)
        faded = (k_ref[rows, :].astype(jnp.float32) * jnp.exp(ending - cumulative)).astype(
            jnp.bfloat16
        )
        local = local * jnp.exp(ending) + mm(v_ref[rows, :], faded, TN)
        ahead = ahead + ending
    send[:width, :] = local.astype(jnp.bfloat16)
    send[width:, :] = jnp.broadcast_to(jnp.exp(ahead), (16, ahead.shape[1])).astype(jnp.bfloat16)
    pl.semaphore_wait(barrier, n - 1)
    copies = state_copies(n, me, 1, send, recv, ssem, rsem)
    for copy in copies:
        copy.start()
    inner = []
    scaled = []
    for b in range(blocks):
        rows = pl.ds(b * BLK, BLK)
        cumulative, middle, _ = decays(g_ref, rows)
        query = q_ref[rows, :].astype(jnp.float32) * scale
        key = k_ref[rows, :].astype(jnp.float32)
        lifted_q = (query * jnp.exp(cumulative - middle)).astype(jnp.bfloat16)
        lifted_k = (key * jnp.exp(middle - cumulative)).astype(jnp.bfloat16)
        scores = jnp.where(causal, mm(lifted_q, lifted_k, NT), 0.0).astype(jnp.bfloat16)
        inner.append(mm(scores, v_ref[rows, :], NN))
        scaled.append((query * jnp.exp(cumulative)).astype(jnp.bfloat16))
    collect(n, me, 1, copies, recv, total, width)
    for b in range(blocks):
        rows = pl.ds(b * BLK, BLK)
        state = (kept[b] + total[...] * jnp.exp(befores[b])).astype(jnp.bfloat16)
        states_ref[b] = state
        mixed_ref[rows, :] = (inner[b] + mm(scaled[b], state, NT)).astype(jnp.bfloat16)


def backward_kernel(
    n,
    scale,
    q_ref,
    k_ref,
    v_ref,
    g_ref,
    d_ref,
    states_ref,
    gq_ref,
    gk_ref,
    gv_ref,
    gg_ref,
    kept,
    total,
    send,
    recv,
    ssem,
    rsem,
):
    me = lax.axis_index("sp")
    barrier = greet(n, me)
    length, width = v_ref.shape
    blocks = length // BLK
    causal = triangle(True)
    local = jnp.zeros(total.shape, jnp.float32)
    after = jnp.zeros((1, q_ref.shape[1]), jnp.float32)
    afters = [None] * blocks
    for b in reversed(range(blocks)):
        rows = pl.ds(b * BLK, BLK)
        cumulative, _, ending = decays(g_ref, rows)
        kept[b] = local
        afters[b] = after
        query = q_ref[rows, :].astype(jnp.float32) * scale
        scaled = (query * jnp.exp(cumulative)).astype(jnp.bfloat16)
        local = local * jnp.exp(ending) + mm(d_ref[rows, :], scaled, TN)
        after = after + ending
    send[:width, :] = local.astype(jnp.bfloat16)
    send[width:, :] = jnp.broadcast_to(jnp.exp(after), (16, after.shape[1])).astype(jnp.bfloat16)
    pl.semaphore_wait(barrier, n - 1)
    copies = state_copies(n, me, -1, send, recv, ssem, rsem)
    for copy in copies:
        copy.start()
    change = []
    key_part = []
    for b in range(blocks):
        rows = pl.ds(b * BLK, BLK)
        cumulative, middle, _ = decays(g_ref, rows)
        query = q_ref[rows, :].astype(jnp.float32) * scale
        key = k_ref[rows, :].astype(jnp.float32)
        value = v_ref[rows, :]
        d_out = d_ref[rows, :]
        rise, fall = jnp.exp(cumulative - middle), jnp.exp(middle - cumulative)
        lifted_q = (query * rise).astype(jnp.bfloat16)
        lifted_k = (key * fall).astype(jnp.bfloat16)
        scores = jnp.where(causal, mm(lifted_q, lifted_k, NT), 0.0).astype(jnp.bfloat16)
        d_scores = jnp.where(causal, mm(d_out, value, NT), 0.0).astype(jnp.bfloat16)
        d_lifted_q = mm(d_scores, lifted_k, NN)
        d_lifted_k = mm(d_scores, lifted_q, TN)
        grown = jnp.exp(cumulative)
        d_carried = mm(d_out, states_ref[b], NN) * grown
        gq_ref[rows, :] = ((d_lifted_q * rise + d_carried) * scale).astype(jnp.bfloat16)
        change.append(
            lifted_q.astype(jnp.float32) * d_lifted_q
            - lifted_k.astype(jnp.float32) * d_lifted_k
            + query * d_carried
        )
        key_part.append(d_lifted_k * fall)
        gg_ref[rows, :] = change[b]
        gv_ref[rows, :] = mm(scores, d_out, TN).astype(gv_ref.dtype)
    collect(n, me, -1, copies, recv, total, width)
    for b in range(blocks):
        rows = pl.ds(b * BLK, BLK)
        cumulative, _, ending = decays(g_ref, rows)
        d_state = kept[b] + total[...] * jnp.exp(afters[b])
        d_rounded = d_state.astype(jnp.bfloat16)
        key = k_ref[rows, :].astype(jnp.float32)
        fade = jnp.exp(ending - cumulative)
        faded = key * fade
        d_faded = mm(v_ref[rows, :], d_rounded, NN)
        gk_ref[rows, :] = (key_part[b] + d_faded * fade).astype(jnp.bfloat16)
        gv_ref[rows, :] = gv_ref[rows, :] + mm(faded.astype(jnp.bfloat16), d_rounded, NT)
        moved = faded * d_faded
        at_end = jnp.sum(moved, axis=0, keepdims=True) + jnp.exp(ending) * jnp.sum(
            states_ref[b].astype(jnp.float32) * d_state, axis=0, keepdims=True
        )
        gg_ref[rows, :] = block_sums(triangle(False), gg_ref[rows, :] - moved) + at_end


def exchange_scratch(n, blocks, width, channels):
    return [
        pltpu.VMEM((blocks, width, channels), jnp.float32),
        pltpu.VMEM((width, channels), jnp.float32),
        pltpu.VMEM((width + 16, channels), jnp.bfloat16),
        pltpu.VMEM((n - 1, width + 16, channels), jnp.bfloat16),
        pltpu.SemaphoreType.DMA((n - 1,)),
        pltpu.SemaphoreType.DMA((n - 1,)),
    ]


def in_vmem(count):
    return [pl.BlockSpec(memory_space=pltpu.VMEM)] * count


def mixer_forward(q, k, v, g, scale):
    n = lax.axis_size("sp")
    length, channels = q.shape
    width = v.shape[1]
    blocks = length // BLK
    return pl.pallas_call(
        functools.partial(forward_kernel, n, scale),
        out_shape=(
            jax.ShapeDtypeStruct((length, width), jnp.bfloat16),
            jax.ShapeDtypeStruct((blocks, width, channels), jnp.bfloat16),
        ),
        in_specs=in_vmem(4),
        out_specs=tuple(in_vmem(2)),
        scratch_shapes=exchange_scratch(n, blocks, width, channels),
        compiler_params=pltpu.CompilerParams(
            collective_id=1, has_side_effects=True, vmem_limit_bytes=16 * 1024 * 1024
        ),
        cost_estimate=pl.CostEstimate(
            flops=4_000_000_000, bytes_accessed=4 * length * width, transcendentals=0
        ),
        name="mixer_forward",
    )(q, k, v, g)


def mixer_backward(q, k, v, g, d, states, scale):
    n = lax.axis_size("sp")
    length, channels = q.shape
    width = v.shape[1]
    blocks = length // BLK
    return pl.pallas_call(
        functools.partial(backward_kernel, n, scale),
        out_shape=(
            jax.ShapeDtypeStruct((length, channels), jnp.bfloat16),
            jax.ShapeDtypeStruct((length, channels), jnp.bfloat16),
            jax.ShapeDtypeStruct((length, width), jnp.float32),
            jax.ShapeDtypeStruct((length, channels), jnp.float32),
        ),
        in_specs=in_vmem(6),
        out_specs=tuple(in_vmem(4)),
        scratch_shapes=exchange_scratch(n, blocks, width, channels),
        compiler_params=pltpu.CompilerParams(
            collective_id=2, has_side_effects=True, vmem_limit_bytes=16 * 1024 * 1024
        ),
        cost_estimate=pl.CostEstimate(
            flops=8_000_000_000, bytes_accessed=4 * length * width, transcendentals=0
        ),
        name="mixer_backward",
    )(q, k, v, g, d, states)


def expert_pass(rows_in, routed_rows, gate_w, up_w, down_w):
    gate_pre = jnp.dot(rows_in, gate_w, preferred_element_type=jnp.float32)
    up_pre = jnp.dot(rows_in, up_w, preferred_element_type=jnp.float32)
    sigmoid_gate = jax.nn.sigmoid(gate_pre)
    active = gate_pre * sigmoid_gate
    hidden = (active * up_pre).astype(jnp.bfloat16)
    d_hidden = lax.dot_general(
        routed_rows, down_w, (((1,), (1,)), ((), ())), preferred_element_type=jnp.float32
    )
    d_gate = (d_hidden * up_pre * sigmoid_gate * (1.0 + gate_pre * (1.0 - sigmoid_gate))).astype(
        jnp.bfloat16
    )
    d_up = (d_hidden * active).astype(jnp.bfloat16)
    rows_first = (((0,), (0,)), ((), ()))
    grad_gate = lax.dot_general(
        rows_in, d_gate, rows_first, preferred_element_type=jnp.float32
    ).astype(jnp.bfloat16)
    grad_up = lax.dot_general(rows_in, d_up, rows_first, preferred_element_type=jnp.float32).astype(
        jnp.bfloat16
    )
    grad_down = lax.dot_general(
        hidden, routed_rows, rows_first, preferred_element_type=jnp.float32
    ).astype(jnp.bfloat16)
    return (grad_gate, grad_up, grad_down, d_gate, d_up)


def local(
    d_out,
    route_expert,
    route_weight,
    expert_inputs,
    w_gate,
    w_up,
    w_down,
    w_out,
    queries,
    keys,
    values,
    log_decay,
):
    tok_rows = d_out.shape[0]
    model_width = d_out.shape[1]
    experts = lax.axis_size("sp")
    capacity = expert_inputs.shape[1] // experts
    flat_experts = route_expert.reshape(-1)
    onehot = (flat_experts[:, None] == jnp.arange(experts, dtype=jnp.int32)[None, :]).astype(
        jnp.int32
    )
    before = jnp.cumsum(onehot, axis=0) - onehot
    rank_slot = jnp.sum(before * onehot, axis=1)
    slot_index = flat_experts * capacity + rank_slot
    quarter = model_width // lax.axis_size("tp")
    column_start = lax.axis_index("tp") * quarter
    own_cols = lax.dynamic_slice_in_dim(d_out, column_start, quarter, 1)
    scaled = (
        jnp.repeat(own_cols, 2, axis=0).astype(jnp.float32) * route_weight.reshape(-1)[:, None]
    ).astype(jnp.bfloat16)
    outbox = (
        jnp.zeros((experts * capacity, own_cols.shape[1]), jnp.bfloat16).at[slot_index].set(scaled)
    )
    outbox = outbox.reshape(experts, capacity, own_cols.shape[1])
    partial_rows = lax.all_to_all(outbox, "sp", split_axis=0, concat_axis=0, tiled=True)
    routed = lax.all_gather(partial_rows, "tp", axis=2, tiled=True)
    routed = routed.reshape(experts * capacity, model_width)
    rows_in = expert_inputs[0]
    gate_w = w_gate[0]
    up_w = w_up[0]
    grad_gate, grad_up, grad_down, d_gate, d_up = expert_pass(
        rows_in, routed, gate_w, up_w, w_down[0]
    )
    partial_terms = lax.dot_general(
        d_gate, gate_w, (((1,), (1,)), ((), ())), preferred_element_type=jnp.float32
    )
    partial_terms = partial_terms + lax.dot_general(
        d_up, up_w, (((1,), (1,)), ((), ())), preferred_element_type=jnp.float32
    )
    rounded = lax.optimization_barrier(partial_terms.astype(jnp.bfloat16)).astype(jnp.float32)
    summed = lax.psum_scatter(rounded.astype(jnp.bfloat16), "tp", scatter_dimension=1, tiled=True)
    returned = lax.all_to_all(
        summed.reshape(experts, capacity, quarter), "sp", split_axis=0, concat_axis=0, tiled=True
    )
    picked = returned.reshape(experts * capacity, quarter)[slot_index].astype(jnp.float32)
    picked = picked.reshape(tok_rows, 2, quarter).sum(axis=1)
    mix_cols = (own_cols.astype(jnp.float32) + picked).astype(jnp.bfloat16)
    mix_grad = lax.all_gather(mix_cols, "tp", axis=1, tiled=True)
    scale_q = queries.shape[2] ** (-0.5)
    q, k, v, g = queries[:, 0], keys[:, 0], values[:, 0], log_decay[:, 0]
    mixed, states = mixer_forward(q, k, v, g, scale_q)
    grad_proj = lax.psum_scatter(
        lax.dot_general(
            mix_grad, mixed, (((0,), (0,)), ((), ())), preferred_element_type=jnp.float32
        ).astype(jnp.bfloat16),
        "sp",
        scatter_dimension=0,
        tiled=True,
    ).astype(jnp.float32)
    d_mixed = jnp.dot(mix_grad, w_out, preferred_element_type=jnp.float32).astype(jnp.bfloat16)
    grad_q, grad_k, grad_v, grad_g = mixer_backward(q, k, v, g, d_mixed, states, scale_q)
    return (
        grad_gate[None],
        grad_up[None],
        grad_down[None],
        grad_proj,
        grad_q[:, None],
        grad_k[:, None],
        grad_v.astype(jnp.bfloat16)[:, None],
        grad_g[:, None],
    )


def solution(mesh):
    return jax.shard_map(
        local,
        mesh=mesh,
        in_specs=(
            P("sp", None),
            P("sp", None),
            P("sp", None),
            P("sp", None, None),
            P("sp", None, "tp"),
            P("sp", None, "tp"),
            P("sp", "tp", None),
            P(None, "tp"),
            P("sp", "tp", None),
            P("sp", "tp", None),
            P("sp", "tp", None),
            P("sp", "tp", None),
        ),
        out_specs=(
            P("sp", None, "tp"),
            P("sp", None, "tp"),
            P("sp", "tp", None),
            P("sp", "tp"),
            P("sp", "tp", None),
            P("sp", "tp", None),
            P("sp", "tp", None),
            P("sp", "tp", None),
        ),
        check_vma=False,
    )
```

```python
import functools

import jax
import jax.numpy as jnp
from jax import lax
from jax.experimental import pallas as pl
from jax.experimental.pallas import tpu as pltpu
from jax.sharding import PartitionSpec as P

BLK = 64


precise = lax.Precision.HIGHEST


MESH = pl.DeviceIdType.MESH
NN = (((1,), (0,)), ((), ()))
NT = (((1,), (1,)), ((), ()))
TN = (((0,), (0,)), ((), ()))


def mm(a, b, dims):
    return lax.dot_general(a, b, dims, preferred_element_type=jnp.float32)


def triangle(lower):
    rows = lax.broadcasted_iota(jnp.int32, (BLK, BLK), 0)
    cols = lax.broadcasted_iota(jnp.int32, (BLK, BLK), 1)
    return rows >= cols if lower else rows <= cols


def block_sums(mask, x):
    return lax.dot_general(
        mask.astype(jnp.float32), x, NN, precision=precise, preferred_element_type=jnp.float32
    )


def decays(g_ref, rows):
    cumulative = block_sums(triangle(True), g_ref[rows, :])
    middle = cumulative[BLK // 2 - 1 : BLK // 2, :]
    ending = cumulative[BLK - 1 : BLK, :]
    return cumulative, middle, ending


def greet(n, me, tp=None):
    barrier = pltpu.get_barrier_semaphore()
    others = [{"sp": lax.rem(me + k, n)} for k in range(1, n)]
    if tp is not None:
        others += [{"tp": other} for other in tp]
    for other in others:
        pl.semaphore_signal(barrier, inc=1, device_id=other, device_id_type=MESH)
    return barrier, len(others)


def route_kernel(n, cap, d_ref, expert_ref, weight_ref, arrived_ref, slot_ref, outbox, ssem, rsem, lsem):
    me = lax.axis_index("sp")
    barrier, greeted = greet(n, me)
    tokens = d_ref.shape[0]
    quarter = outbox.shape[2]
    start = pl.multiple_of(lax.axis_index("tp") * quarter, quarter)
    own = d_ref[:, pl.ds(start, quarter)].astype(jnp.float32)
    kinds = lax.broadcasted_iota(jnp.int32, (n, tokens), 0)
    named = [(kinds == expert_ref[j : j + 1, :]).astype(jnp.float32) for j in range(2)]
    earlier = lax.broadcasted_iota(jnp.int32, (tokens, tokens), 0) < lax.broadcasted_iota(
        jnp.int32, (tokens, tokens), 1
    )
    before = mm((named[0] + named[1]).astype(jnp.bfloat16), earlier.astype(jnp.bfloat16), NN)
    scaled = []
    slots = []
    for j in range(2):
        rank = jnp.sum(before * named[j], axis=0, keepdims=True).astype(jnp.int32)
        slots.append(expert_ref[j : j + 1, :] * cap + rank)
        slot_ref[j : j + 1, :] = slots[j]
        scaled.append((own * weight_ref[:, j : j + 1]).astype(jnp.bfloat16))
    places = lax.broadcasted_iota(jnp.int32, (cap, tokens), 0)
    for e in range(n):
        rows = jnp.zeros((cap, quarter), jnp.float32)
        for j in range(2):
            picks = (slots[j] - e * cap == places).astype(jnp.float32).astype(jnp.bfloat16)
            rows = rows + mm(picks, scaled[j], NN)
        outbox[e] = rows.astype(jnp.bfloat16)
    pl.semaphore_wait(barrier, greeted)
    exchange(n, me, outbox, arrived_ref, ssem, rsem, lsem)


def exchange(n, me, source, target, ssem, rsem, lsem):
    copies = []
    for k in range(1, n):
        peer = lax.rem(me + k, n)
        copies.append(
            pltpu.make_async_remote_copy(
                src_ref=source.at[peer],
                dst_ref=target.at[me],
                send_sem=ssem.at[k - 1],
                recv_sem=rsem.at[k - 1],
                device_id={"sp": peer},
                device_id_type=MESH,
            )
        )
    for copy in copies:
        copy.start()
    stays = pltpu.make_async_copy(source.at[me], target.at[me], lsem)
    stays.start()
    stays.wait()
    for copy in copies:
        copy.wait()


def return_kernel(
    n, tp, cap, sums_ref, slot_ref, d_ref, gathered_ref, back, ssem, rsem, lsem, tsend, trecv
):
    me = lax.axis_index("sp")
    col = lax.axis_index("tp")
    partner = col + 1 - 2 * lax.rem(col, 2)
    far = [lax.rem(col + 2 * s, tp) for s in range(1, tp // 2)]
    barrier, greeted = greet(n, me, [partner] + far)
    pl.semaphore_wait(barrier, greeted)
    exchange(n, me, sums_ref, back, ssem, rsem, lsem)
    tokens = d_ref.shape[0]
    quarter = back.shape[2]
    start = pl.multiple_of(col * quarter, quarter)
    places = lax.broadcasted_iota(jnp.int32, (cap, tokens), 0)
    picked = jnp.zeros((tokens, quarter), jnp.float32)
    for e in range(n):
        here = jnp.zeros((cap, tokens), jnp.float32)
        for j in range(2):
            here = here + (slot_ref[j : j + 1, :] - e * cap == places).astype(jnp.float32)
        picked = picked + mm(here.astype(jnp.bfloat16), back[e], TN)
    own = d_ref[:, pl.ds(start, quarter)].astype(jnp.float32)
    gathered_ref[col] = (own + picked).astype(jnp.bfloat16)

    def send(block, slot, target):
        return pltpu.make_async_remote_copy(
            src_ref=gathered_ref.at[block],
            dst_ref=gathered_ref.at[block],
            send_sem=tsend.at[slot],
            recv_sem=trecv.at[slot],
            device_id={"tp": target},
            device_id_type=MESH,
        )

    across = [send(col, s + 1, far[s]) for s in range(len(far))]
    beside = send(col, 0, partner)
    for copy in across:
        copy.start()
    beside.start()
    passed = []
    for s in range(len(far)):
        across[s].wait_recv()
        block = lax.rem(col - 2 * (s + 1) + tp, tp)
        passed.append(send(block, tp // 2 + s, partner))
        passed[s].start()
    for copy in across:
        copy.wait_send()
    beside.wait()
    for copy in passed:
        copy.wait()


def state_copies(n, me, step, send_ref, recv_ref, send_sem, recv_sem):
    return [
        pltpu.make_async_remote_copy(
            src_ref=send_ref,
            dst_ref=recv_ref.at[k - 1],
            send_sem=send_sem.at[k - 1],
            recv_sem=recv_sem.at[k - 1],
            device_id={"sp": lax.rem(me + step * k + n, n)},
            device_id_type=MESH,
        )
        for k in range(1, n)
    ]


def collect(n, me, step, copies, recv_ref, total, width):
    total[...] = jnp.zeros_like(total)
    for k in range(n - 1, 0, -1):
        copies[k - 1].wait()
        source = me - step * k
        reached = jnp.logical_and(source >= 0, source < n)

        @pl.when(reached)
        def _():
            factor = recv_ref[k - 1, width : width + 1, :].astype(jnp.float32)
            total[...] = total[...] * factor + recv_ref[k - 1, :width, :].astype(jnp.float32)


def forward_kernel(
    n, scale, q_ref, k_ref, v_ref, g_ref, mixed_ref, states_ref, kept, total, send, recv, ssem, rsem
):
    me = lax.axis_index("sp")
    barrier, greeted = greet(n, me)
    length, width = v_ref.shape
    blocks = length // BLK
    causal = triangle(True)
    local = jnp.zeros(total.shape, jnp.float32)
    ahead = jnp.zeros((1, q_ref.shape[1]), jnp.float32)
    befores = []
    for b in range(blocks):
        rows = pl.ds(b * BLK, BLK)
        cumulative, _, ending = decays(g_ref, rows)
        kept[b] = local
        befores.append(ahead)
        faded = (k_ref[rows, :].astype(jnp.float32) * jnp.exp(ending - cumulative)).astype(
            jnp.bfloat16
        )
        local = local * jnp.exp(ending) + mm(v_ref[rows, :], faded, TN)
        ahead = ahead + ending
    send[:width, :] = local.astype(jnp.bfloat16)
    send[width:, :] = jnp.broadcast_to(jnp.exp(ahead), (16, ahead.shape[1])).astype(jnp.bfloat16)
    pl.semaphore_wait(barrier, greeted)
    copies = state_copies(n, me, 1, send, recv, ssem, rsem)
    for copy in copies:
        copy.start()
    inner = []
    scaled = []
    for b in range(blocks):
        rows = pl.ds(b * BLK, BLK)
        cumulative, middle, _ = decays(g_ref, rows)
        query = q_ref[rows, :].astype(jnp.float32) * scale
        key = k_ref[rows, :].astype(jnp.float32)
        lifted_q = (query * jnp.exp(cumulative - middle)).astype(jnp.bfloat16)
        lifted_k = (key * jnp.exp(middle - cumulative)).astype(jnp.bfloat16)
        scores = jnp.where(causal, mm(lifted_q, lifted_k, NT), 0.0).astype(jnp.bfloat16)
        inner.append(mm(scores, v_ref[rows, :], NN))
        scaled.append((query * jnp.exp(cumulative)).astype(jnp.bfloat16))
    collect(n, me, 1, copies, recv, total, width)
    for b in range(blocks):
        rows = pl.ds(b * BLK, BLK)
        state = (kept[b] + total[...] * jnp.exp(befores[b])).astype(jnp.bfloat16)
        states_ref[b] = state
        mixed_ref[rows, :] = (inner[b] + mm(scaled[b], state, NT)).astype(jnp.bfloat16)


def backward_kernel(
    n,
    scale,
    q_ref,
    k_ref,
    v_ref,
    g_ref,
    grad_ref,
    w_ref,
    mixed_ref,
    states_ref,
    gq_ref,
    gk_ref,
    gv_ref,
    gg_ref,
    proj_ref,
    kept,
    total,
    send,
    recv,
    ssem,
    rsem,
    d_ref,
    part,
    parts_in,
    psend,
    precv,
):
    me = lax.axis_index("sp")
    barrier, greeted = greet(n, me)
    length, width = v_ref.shape
    blocks = length // BLK
    causal = triangle(True)
    local = jnp.zeros(total.shape, jnp.float32)
    pieces, _, quarter = grad_ref.shape
    d_mixed = jnp.zeros((length, width), jnp.float32)
    for p in range(pieces):
        d_mixed = d_mixed + mm(grad_ref[p], w_ref[p * quarter : (p + 1) * quarter, :], NN)
    d_ref[...] = d_mixed.astype(jnp.bfloat16)
    after = jnp.zeros((1, q_ref.shape[1]), jnp.float32)
    afters = [None] * blocks
    for b in reversed(range(blocks)):
        rows = pl.ds(b * BLK, BLK)
        cumulative, _, ending = decays(g_ref, rows)
        kept[b] = local
        afters[b] = after
        query = q_ref[rows, :].astype(jnp.float32) * scale
        scaled = (query * jnp.exp(cumulative)).astype(jnp.bfloat16)
        local = local * jnp.exp(ending) + mm(d_ref[rows, :], scaled, TN)
        after = after + ending
    send[:width, :] = local.astype(jnp.bfloat16)
    send[width:, :] = jnp.broadcast_to(jnp.exp(after), (16, after.shape[1])).astype(jnp.bfloat16)
    pl.semaphore_wait(barrier, greeted)
    copies = state_copies(n, me, -1, send, recv, ssem, rsem)
    for copy in copies:
        copy.start()
    share = part.shape[1]
    per = quarter // share
    for p in range(pieces):
        product = mm(grad_ref[p], mixed_ref[...], TN).astype(jnp.bfloat16)
        for i in range(per):
            part[p * per + i] = product[i * share : (i + 1) * share, :]
    shares = []
    for s in range(1, n):
        peer = lax.rem(me + s, n)
        shares.append(
            pltpu.make_async_remote_copy(
                src_ref=part.at[peer],
                dst_ref=parts_in.at[s - 1],
                send_sem=psend.at[s - 1],
                recv_sem=precv.at[s - 1],
                device_id={"sp": peer},
                device_id_type=MESH,
            )
        )
        shares[-1].start()
    change = []
    key_part = []
    for b in range(blocks):
        rows = pl.ds(b * BLK, BLK)
        cumulative, middle, _ = decays(g_ref, rows)
        query = q_ref[rows, :].astype(jnp.float32) * scale
        key = k_ref[rows, :].astype(jnp.float32)
        value = v_ref[rows, :]
        d_out = d_ref[rows, :]
        rise, fall = jnp.exp(cumulative - middle), jnp.exp(middle - cumulative)
        lifted_q = (query * rise).astype(jnp.bfloat16)
        lifted_k = (key * fall).astype(jnp.bfloat16)
        scores = jnp.where(causal, mm(lifted_q, lifted_k, NT), 0.0).astype(jnp.bfloat16)
        d_scores = jnp.where(causal, mm(d_out, value, NT), 0.0).astype(jnp.bfloat16)
        d_lifted_q = mm(d_scores, lifted_k, NN)
        d_lifted_k = mm(d_scores, lifted_q, TN)
        grown = jnp.exp(cumulative)
        d_carried = mm(d_out, states_ref[b], NN) * grown
        gq_ref[rows, :] = ((d_lifted_q * rise + d_carried) * scale).astype(jnp.bfloat16)
        change.append(
            lifted_q.astype(jnp.float32) * d_lifted_q
            - lifted_k.astype(jnp.float32) * d_lifted_k
            + query * d_carried
        )
        key_part.append(d_lifted_k * fall)
        gg_ref[rows, :] = change[b]
        gv_ref[rows, :] = mm(scores, d_out, TN).astype(gv_ref.dtype)
    collect(n, me, -1, copies, recv, total, width)
    for b in range(blocks):
        rows = pl.ds(b * BLK, BLK)
        cumulative, _, ending = decays(g_ref, rows)
        d_state = kept[b] + total[...] * jnp.exp(afters[b])
        d_rounded = d_state.astype(jnp.bfloat16)
        key = k_ref[rows, :].astype(jnp.float32)
        fade = jnp.exp(ending - cumulative)
        faded = key * fade
        d_faded = mm(v_ref[rows, :], d_rounded, NN)
        gk_ref[rows, :] = (key_part[b] + d_faded * fade).astype(jnp.bfloat16)
        gv_ref[rows, :] = gv_ref[rows, :] + mm(faded.astype(jnp.bfloat16), d_rounded, NT)
        moved = faded * d_faded
        at_end = jnp.sum(moved, axis=0, keepdims=True) + jnp.exp(ending) * jnp.sum(
            states_ref[b].astype(jnp.float32) * d_state, axis=0, keepdims=True
        )
        gg_ref[rows, :] = block_sums(triangle(False), gg_ref[rows, :] - moved) + at_end
    summed = part[me].astype(jnp.float32)
    for s in range(1, n):
        shares[s - 1].wait()
        summed = summed + parts_in[s - 1].astype(jnp.float32)
    proj_ref[...] = summed


def exchange_scratch(n, blocks, width, channels):
    return [
        pltpu.VMEM((blocks, width, channels), jnp.float32),
        pltpu.VMEM((width, channels), jnp.float32),
        pltpu.VMEM((width + 16, channels), jnp.bfloat16),
        pltpu.VMEM((n - 1, width + 16, channels), jnp.bfloat16),
        pltpu.SemaphoreType.DMA((n - 1,)),
        pltpu.SemaphoreType.DMA((n - 1,)),
    ]


def in_vmem(count):
    return [pl.BlockSpec(memory_space=pltpu.VMEM)] * count


def mixer_forward(q, k, v, g, scale):
    n = lax.axis_size("sp")
    length, channels = q.shape
    width = v.shape[1]
    blocks = length // BLK
    return pl.pallas_call(
        functools.partial(forward_kernel, n, scale),
        out_shape=(
            jax.ShapeDtypeStruct((length, width), jnp.bfloat16),
            jax.ShapeDtypeStruct((blocks, width, channels), jnp.bfloat16),
        ),
        in_specs=in_vmem(4),
        out_specs=tuple(in_vmem(2)),
        scratch_shapes=exchange_scratch(n, blocks, width, channels),
        compiler_params=pltpu.CompilerParams(
            collective_id=1, has_side_effects=True, vmem_limit_bytes=16 * 1024 * 1024
        ),
        cost_estimate=pl.CostEstimate(
            flops=4_000_000_000, bytes_accessed=4 * length * width, transcendentals=0
        ),
        name="mixer_forward",
    )(q, k, v, g)


def mixer_backward(q, k, v, g, gathered, w_out, mixed, states, scale):
    n = lax.axis_size("sp")
    length, channels = q.shape
    width = v.shape[1]
    blocks = length // BLK
    share = w_out.shape[0] // n
    return pl.pallas_call(
        functools.partial(backward_kernel, n, scale),
        out_shape=(
            jax.ShapeDtypeStruct((length, channels), jnp.bfloat16),
            jax.ShapeDtypeStruct((length, channels), jnp.bfloat16),
            jax.ShapeDtypeStruct((length, width), jnp.float32),
            jax.ShapeDtypeStruct((length, channels), jnp.float32),
            jax.ShapeDtypeStruct((share, width), jnp.float32),
        ),
        in_specs=in_vmem(8),
        out_specs=tuple(in_vmem(5)),
        scratch_shapes=exchange_scratch(n, blocks, width, channels)
        + [
            pltpu.VMEM((length, width), jnp.bfloat16),
            pltpu.VMEM((n, share, width), jnp.bfloat16),
            pltpu.VMEM((n - 1, share, width), jnp.bfloat16),
            pltpu.SemaphoreType.DMA((n - 1,)),
            pltpu.SemaphoreType.DMA((n - 1,)),
        ],
        compiler_params=pltpu.CompilerParams(
            collective_id=2, has_side_effects=True, vmem_limit_bytes=24 * 1024 * 1024
        ),
        cost_estimate=pl.CostEstimate(
            flops=8_000_000_000, bytes_accessed=4 * length * width, transcendentals=0
        ),
        name="mixer_backward",
    )(q, k, v, g, gathered, w_out, mixed, states)


def route_out(d_out, route_expert, route_weight, capacity):
    n, tp = lax.axis_size("sp"), lax.axis_size("tp")
    tokens, model_width = d_out.shape
    quarter = model_width // tp
    return pl.pallas_call(
        functools.partial(route_kernel, n, capacity),
        out_shape=(
            jax.ShapeDtypeStruct((n, capacity, quarter), jnp.bfloat16),
            jax.ShapeDtypeStruct((2, tokens), jnp.int32),
        ),
        in_specs=in_vmem(3),
        out_specs=tuple(in_vmem(2)),
        scratch_shapes=[
            pltpu.VMEM((n, capacity, quarter), jnp.bfloat16),
            pltpu.SemaphoreType.DMA((n - 1,)),
            pltpu.SemaphoreType.DMA((n - 1,)),
            pltpu.SemaphoreType.DMA,
        ],
        compiler_params=pltpu.CompilerParams(
            collective_id=3, has_side_effects=True, vmem_limit_bytes=24 * 1024 * 1024
        ),
        cost_estimate=pl.CostEstimate(
            flops=8_000_000_000, bytes_accessed=4 * tokens * quarter, transcendentals=0
        ),
        name="route_out",
    )(d_out, route_expert.T, route_weight)


def route_back(summed, slots, d_out):
    n, tp = lax.axis_size("sp"), lax.axis_size("tp")
    capacity, quarter = summed.shape[1:]
    tokens = d_out.shape[0]
    return pl.pallas_call(
        functools.partial(return_kernel, n, tp, capacity),
        out_shape=jax.ShapeDtypeStruct((tp, tokens, quarter), jnp.bfloat16),
        in_specs=in_vmem(3),
        out_specs=in_vmem(1)[0],
        scratch_shapes=[
            pltpu.VMEM((n, capacity, quarter), jnp.bfloat16),
            pltpu.SemaphoreType.DMA((n - 1,)),
            pltpu.SemaphoreType.DMA((n - 1,)),
            pltpu.SemaphoreType.DMA,
            pltpu.SemaphoreType.DMA((tp,)),
            pltpu.SemaphoreType.DMA((tp,)),
        ],
        compiler_params=pltpu.CompilerParams(
            collective_id=4, has_side_effects=True, vmem_limit_bytes=24 * 1024 * 1024
        ),
        cost_estimate=pl.CostEstimate(
            flops=8_000_000_000, bytes_accessed=4 * tokens * quarter, transcendentals=0
        ),
        name="route_back",
    )(summed, slots, d_out)


def expert_pass(rows_in, routed_rows, gate_w, up_w, down_w):
    gate_pre = jnp.dot(rows_in, gate_w, preferred_element_type=jnp.float32)
    up_pre = jnp.dot(rows_in, up_w, preferred_element_type=jnp.float32)
    sigmoid_gate = jax.nn.sigmoid(gate_pre)
    active = gate_pre * sigmoid_gate
    hidden = (active * up_pre).astype(jnp.bfloat16)
    d_hidden = lax.dot_general(
        routed_rows, down_w, (((1,), (1,)), ((), ())), preferred_element_type=jnp.float32
    )
    d_gate = (d_hidden * up_pre * sigmoid_gate * (1.0 + gate_pre * (1.0 - sigmoid_gate))).astype(
        jnp.bfloat16
    )
    d_up = (d_hidden * active).astype(jnp.bfloat16)
    rows_first = (((0,), (0,)), ((), ()))
    grad_gate = lax.dot_general(
        rows_in, d_gate, rows_first, preferred_element_type=jnp.float32
    ).astype(jnp.bfloat16)
    grad_up = lax.dot_general(rows_in, d_up, rows_first, preferred_element_type=jnp.float32).astype(
        jnp.bfloat16
    )
    grad_down = lax.dot_general(
        hidden, routed_rows, rows_first, preferred_element_type=jnp.float32
    ).astype(jnp.bfloat16)
    return (grad_gate, grad_up, grad_down, d_gate, d_up)


def local(
    d_out,
    route_expert,
    route_weight,
    expert_inputs,
    w_gate,
    w_up,
    w_down,
    w_out,
    queries,
    keys,
    values,
    log_decay,
):
    model_width = d_out.shape[1]
    experts = lax.axis_size("sp")
    capacity = expert_inputs.shape[1] // experts
    quarter = model_width // lax.axis_size("tp")
    partial_rows, slots = route_out(d_out, route_expert, route_weight, capacity)
    routed = lax.all_gather(partial_rows, "tp", axis=2, tiled=True)
    routed = routed.reshape(experts * capacity, model_width)
    rows_in = expert_inputs[0]
    gate_w = w_gate[0]
    up_w = w_up[0]
    grad_gate, grad_up, grad_down, d_gate, d_up = expert_pass(
        rows_in, routed, gate_w, up_w, w_down[0]
    )
    partial_terms = lax.dot_general(
        d_gate, gate_w, (((1,), (1,)), ((), ())), preferred_element_type=jnp.float32
    )
    partial_terms = partial_terms + lax.dot_general(
        d_up, up_w, (((1,), (1,)), ((), ())), preferred_element_type=jnp.float32
    )
    rounded = lax.optimization_barrier(partial_terms.astype(jnp.bfloat16)).astype(jnp.float32)
    summed = lax.psum_scatter(rounded.astype(jnp.bfloat16), "tp", scatter_dimension=1, tiled=True)
    scale_q = queries.shape[2] ** (-0.5)
    q, k, v, g = queries[:, 0], keys[:, 0], values[:, 0], log_decay[:, 0]
    mixed, states = mixer_forward(q, k, v, g, scale_q)
    summed, mixed, grad_gate, grad_up, grad_down = lax.optimization_barrier(
        (summed, mixed, grad_gate, grad_up, grad_down)
    )
    gathered = route_back(summed.reshape(experts, capacity, quarter), slots, d_out)
    grad_q, grad_k, grad_v, grad_g, grad_proj = mixer_backward(
        q, k, v, g, gathered, w_out, mixed, states, scale_q
    )
    return (
        grad_gate[None],
        grad_up[None],
        grad_down[None],
        grad_proj,
        grad_q[:, None],
        grad_k[:, None],
        grad_v.astype(jnp.bfloat16)[:, None],
        grad_g[:, None],
    )


def solution(mesh):
    return jax.shard_map(
        local,
        mesh=mesh,
        in_specs=(
            P("sp", None),
            P("sp", None),
            P("sp", None),
            P("sp", None, None),
            P("sp", None, "tp"),
            P("sp", None, "tp"),
            P("sp", "tp", None),
            P(None, "tp"),
            P("sp", "tp", None),
            P("sp", "tp", None),
            P("sp", "tp", None),
            P("sp", "tp", None),
        ),
        out_specs=(
            P("sp", None, "tp"),
            P("sp", None, "tp"),
            P("sp", "tp", None),
            P("sp", "tp"),
            P("sp", "tp", None),
            P("sp", "tp", None),
            P("sp", "tp", None),
            P("sp", "tp", None),
        ),
        check_vma=False,
    )
```

```python
import functools

import jax
import jax.numpy as jnp
from jax import lax
from jax.experimental import pallas as pl
from jax.experimental.pallas import tpu as pltpu
from jax.sharding import PartitionSpec as P

BLK = 64


precise = lax.Precision.HIGHEST


MESH = pl.DeviceIdType.MESH
NN = (((1,), (0,)), ((), ()))
NT = (((1,), (1,)), ((), ()))
TN = (((0,), (0,)), ((), ()))


def mm(a, b, dims):
    return lax.dot_general(a, b, dims, preferred_element_type=jnp.float32)


def triangle(lower):
    rows = lax.broadcasted_iota(jnp.int32, (BLK, BLK), 0)
    cols = lax.broadcasted_iota(jnp.int32, (BLK, BLK), 1)
    return rows >= cols if lower else rows <= cols


def block_sums(mask, x):
    return lax.dot_general(
        mask.astype(jnp.float32), x, NN, precision=precise, preferred_element_type=jnp.float32
    )


def decays(g_ref, rows):
    cumulative = block_sums(triangle(True), g_ref[rows, :])
    middle = cumulative[BLK // 2 - 1 : BLK // 2, :]
    ending = cumulative[BLK - 1 : BLK, :]
    return cumulative, middle, ending


def greet(n, me, tp=None):
    barrier = pltpu.get_barrier_semaphore()
    others = [{"sp": lax.rem(me + k, n)} for k in range(1, n)]
    if tp is not None:
        others += [{"tp": other} for other in tp]
    for other in others:
        pl.semaphore_signal(barrier, inc=1, device_id=other, device_id_type=MESH)
    return barrier, len(others)


def route_kernel(
    n,
    tp,
    cap,
    d_ref,
    expert_ref,
    weight_ref,
    routed_ref,
    slot_ref,
    outbox,
    ssem,
    rsem,
    lsem,
    tsend,
    trecv,
):
    me = lax.axis_index("sp")
    col = lax.axis_index("tp")
    partner = col + 1 - 2 * lax.rem(col, 2)
    far = [lax.rem(col + 2 * s, tp) for s in range(1, tp // 2)]
    barrier, greeted = greet(n, me, [partner] + far)
    tokens = d_ref.shape[0]
    quarter = outbox.shape[2]
    start = pl.multiple_of(lax.axis_index("tp") * quarter, quarter)
    own = d_ref[:, pl.ds(start, quarter)].astype(jnp.float32)
    kinds = lax.broadcasted_iota(jnp.int32, (n, tokens), 0)
    named = [(kinds == expert_ref[j : j + 1, :]).astype(jnp.float32) for j in range(2)]
    earlier = lax.broadcasted_iota(jnp.int32, (tokens, tokens), 0) < lax.broadcasted_iota(
        jnp.int32, (tokens, tokens), 1
    )
    before = mm((named[0] + named[1]).astype(jnp.bfloat16), earlier.astype(jnp.bfloat16), NN)
    scaled = []
    slots = []
    for j in range(2):
        rank = jnp.sum(before * named[j], axis=0, keepdims=True).astype(jnp.int32)
        slots.append(expert_ref[j : j + 1, :] * cap + rank)
        slot_ref[j : j + 1, :] = slots[j]
        scaled.append((own * weight_ref[:, j : j + 1]).astype(jnp.bfloat16))
    places = lax.broadcasted_iota(jnp.int32, (cap, tokens), 0)
    for e in range(n):
        rows = jnp.zeros((cap, quarter), jnp.float32)
        for j in range(2):
            picks = (slots[j] - e * cap == places).astype(jnp.float32).astype(jnp.bfloat16)
            rows = rows + mm(picks, scaled[j], NN)
        outbox[e] = rows.astype(jnp.bfloat16)
    pl.semaphore_wait(barrier, greeted)

    def place(row, column):
        return routed_ref.at[row, :, pl.ds(pl.multiple_of(column * quarter, quarter), quarter)]

    copies = []
    for k in range(1, n):
        peer = lax.rem(me + k, n)
        copies.append(
            pltpu.make_async_remote_copy(
                src_ref=outbox.at[peer],
                dst_ref=place(me, col),
                send_sem=ssem.at[k - 1],
                recv_sem=rsem.at[k - 1],
                device_id={"sp": peer},
                device_id_type=MESH,
            )
        )
        copies[-1].start()
    stays = pltpu.make_async_copy(outbox.at[me], place(me, col), lsem)
    stays.start()

    def send(k, column, slot, target):
        row = lax.rem(me - k + n, n)
        return pltpu.make_async_remote_copy(
            src_ref=place(row, column),
            dst_ref=place(row, column),
            send_sem=tsend.at[k, slot],
            recv_sem=trecv.at[k, slot],
            device_id={"tp": target},
            device_id_type=MESH,
        )

    across, beside, passed = [], [], []

    def pass_on(k):
        for s in range(len(far)):
            across[k][s].wait_recv()
            column = lax.rem(col - 2 * (s + 1) + tp, tp)
            passed.append(send(k, column, tp // 2 + s, partner))
            passed[-1].start()

    for k in range(n):
        if k == 0:
            stays.wait()
        else:
            copies[k - 1].wait_recv()
        across.append([send(k, col, s + 1, far[s]) for s in range(len(far))])
        for copy in across[k]:
            copy.start()
        beside.append(send(k, col, 0, partner))
        beside[k].start()
        if k > 1:
            pass_on(k - 2)
    for k in range(max(n - 2, 0), n):
        pass_on(k)
    for copy in copies:
        copy.wait_send()
    for row in across:
        for copy in row:
            copy.wait_send()
    for copy in beside + passed:
        copy.wait()


def exchange(n, me, source, target, ssem, rsem, lsem):
    copies = []
    for k in range(1, n):
        peer = lax.rem(me + k, n)
        copies.append(
            pltpu.make_async_remote_copy(
                src_ref=source.at[peer],
                dst_ref=target.at[me],
                send_sem=ssem.at[k - 1],
                recv_sem=rsem.at[k - 1],
                device_id={"sp": peer},
                device_id_type=MESH,
            )
        )
    for copy in copies:
        copy.start()
    stays = pltpu.make_async_copy(source.at[me], target.at[me], lsem)
    stays.start()
    stays.wait()
    for copy in copies:
        copy.wait()


def return_kernel(
    n, tp, cap, sums_ref, slot_ref, d_ref, gathered_ref, back, ssem, rsem, lsem, tsend, trecv
):
    me = lax.axis_index("sp")
    col = lax.axis_index("tp")
    partner = col + 1 - 2 * lax.rem(col, 2)
    far = [lax.rem(col + 2 * s, tp) for s in range(1, tp // 2)]
    barrier, greeted = greet(n, me, [partner] + far)
    pl.semaphore_wait(barrier, greeted)
    exchange(n, me, sums_ref, back, ssem, rsem, lsem)
    tokens = d_ref.shape[0]
    quarter = back.shape[2]
    start = pl.multiple_of(col * quarter, quarter)
    places = lax.broadcasted_iota(jnp.int32, (cap, tokens), 0)
    picked = jnp.zeros((tokens, quarter), jnp.float32)
    for e in range(n):
        here = jnp.zeros((cap, tokens), jnp.float32)
        for j in range(2):
            here = here + (slot_ref[j : j + 1, :] - e * cap == places).astype(jnp.float32)
        picked = picked + mm(here.astype(jnp.bfloat16), back[e], TN)
    own = d_ref[:, pl.ds(start, quarter)].astype(jnp.float32)
    gathered_ref[col] = (own + picked).astype(jnp.bfloat16)

    def send(block, slot, target):
        return pltpu.make_async_remote_copy(
            src_ref=gathered_ref.at[block],
            dst_ref=gathered_ref.at[block],
            send_sem=tsend.at[slot],
            recv_sem=trecv.at[slot],
            device_id={"tp": target},
            device_id_type=MESH,
        )

    across = [send(col, s + 1, far[s]) for s in range(len(far))]
    beside = send(col, 0, partner)
    for copy in across:
        copy.start()
    beside.start()
    passed = []
    for s in range(len(far)):
        across[s].wait_recv()
        block = lax.rem(col - 2 * (s + 1) + tp, tp)
        passed.append(send(block, tp // 2 + s, partner))
        passed[s].start()
    for copy in across:
        copy.wait_send()
    beside.wait()
    for copy in passed:
        copy.wait()


def state_copies(n, me, step, send_ref, recv_ref, send_sem, recv_sem):
    return [
        pltpu.make_async_remote_copy(
            src_ref=send_ref,
            dst_ref=recv_ref.at[k - 1],
            send_sem=send_sem.at[k - 1],
            recv_sem=recv_sem.at[k - 1],
            device_id={"sp": lax.rem(me + step * k + n, n)},
            device_id_type=MESH,
        )
        for k in range(1, n)
    ]


def collect(n, me, step, copies, recv_ref, total, width):
    total[...] = jnp.zeros_like(total)
    for k in range(n - 1, 0, -1):
        copies[k - 1].wait()
        source = me - step * k
        reached = jnp.logical_and(source >= 0, source < n)

        @pl.when(reached)
        def _():
            factor = recv_ref[k - 1, width : width + 1, :].astype(jnp.float32)
            total[...] = total[...] * factor + recv_ref[k - 1, :width, :].astype(jnp.float32)


def forward_kernel(
    n, scale, q_ref, k_ref, v_ref, g_ref, mixed_ref, states_ref, kept, total, send, recv, ssem, rsem
):
    me = lax.axis_index("sp")
    barrier, greeted = greet(n, me)
    length, width = v_ref.shape
    blocks = length // BLK
    causal = triangle(True)
    local = jnp.zeros(total.shape, jnp.float32)
    ahead = jnp.zeros((1, q_ref.shape[1]), jnp.float32)
    befores = []
    for b in range(blocks):
        rows = pl.ds(b * BLK, BLK)
        cumulative, _, ending = decays(g_ref, rows)
        kept[b] = local
        befores.append(ahead)
        faded = (k_ref[rows, :].astype(jnp.float32) * jnp.exp(ending - cumulative)).astype(
            jnp.bfloat16
        )
        local = local * jnp.exp(ending) + mm(v_ref[rows, :], faded, TN)
        ahead = ahead + ending
    send[:width, :] = local.astype(jnp.bfloat16)
    send[width:, :] = jnp.broadcast_to(jnp.exp(ahead), (16, ahead.shape[1])).astype(jnp.bfloat16)
    pl.semaphore_wait(barrier, greeted)
    copies = state_copies(n, me, 1, send, recv, ssem, rsem)
    for copy in copies:
        copy.start()
    inner = []
    scaled = []
    for b in range(blocks):
        rows = pl.ds(b * BLK, BLK)
        cumulative, middle, _ = decays(g_ref, rows)
        query = q_ref[rows, :].astype(jnp.float32) * scale
        key = k_ref[rows, :].astype(jnp.float32)
        lifted_q = (query * jnp.exp(cumulative - middle)).astype(jnp.bfloat16)
        lifted_k = (key * jnp.exp(middle - cumulative)).astype(jnp.bfloat16)
        scores = jnp.where(causal, mm(lifted_q, lifted_k, NT), 0.0).astype(jnp.bfloat16)
        inner.append(mm(scores, v_ref[rows, :], NN))
        scaled.append((query * jnp.exp(cumulative)).astype(jnp.bfloat16))
    collect(n, me, 1, copies, recv, total, width)
    for b in range(blocks):
        rows = pl.ds(b * BLK, BLK)
        state = (kept[b] + total[...] * jnp.exp(befores[b])).astype(jnp.bfloat16)
        states_ref[b] = state
        mixed_ref[rows, :] = (inner[b] + mm(scaled[b], state, NT)).astype(jnp.bfloat16)


def backward_kernel(
    n,
    scale,
    q_ref,
    k_ref,
    v_ref,
    g_ref,
    grad_ref,
    w_ref,
    mixed_ref,
    states_ref,
    gq_ref,
    gk_ref,
    gv_ref,
    gg_ref,
    proj_ref,
    kept,
    total,
    send,
    recv,
    ssem,
    rsem,
    d_ref,
    part,
    pair_in,
    pair,
    parts_in,
    psend,
    precv,
):
    me = lax.axis_index("sp")
    barrier, greeted = greet(n, me)
    length, width = v_ref.shape
    blocks = length // BLK
    causal = triangle(True)
    local = jnp.zeros(total.shape, jnp.float32)
    pieces, _, quarter = grad_ref.shape
    d_mixed = jnp.zeros((length, width), jnp.float32)
    for p in range(pieces):
        d_mixed = d_mixed + mm(grad_ref[p], w_ref[p * quarter : (p + 1) * quarter, :], NN)
    d_ref[...] = d_mixed.astype(jnp.bfloat16)
    after = jnp.zeros((1, q_ref.shape[1]), jnp.float32)
    afters = [None] * blocks
    for b in reversed(range(blocks)):
        rows = pl.ds(b * BLK, BLK)
        cumulative, _, ending = decays(g_ref, rows)
        kept[b] = local
        afters[b] = after
        query = q_ref[rows, :].astype(jnp.float32) * scale
        scaled = (query * jnp.exp(cumulative)).astype(jnp.bfloat16)
        local = local * jnp.exp(ending) + mm(d_ref[rows, :], scaled, TN)
        after = after + ending
    send[:width, :] = local.astype(jnp.bfloat16)
    send[width:, :] = jnp.broadcast_to(jnp.exp(after), (16, after.shape[1])).astype(jnp.bfloat16)
    pl.semaphore_wait(barrier, greeted)
    copies = state_copies(n, me, -1, send, recv, ssem, rsem)
    for copy in copies:
        copy.start()
    half, share = part.shape[1:3]
    per = quarter // share
    for p in range(pieces):
        product = mm(grad_ref[p], mixed_ref[...], TN).astype(jnp.bfloat16)
        for i in range(per):
            at = p * per + i
            part[at % 2, at // 2] = product[i * share : (i + 1) * share, :]
    parity = lax.rem(me, 2)
    mine = me // 2
    pairing = pltpu.make_async_remote_copy(
        src_ref=part.at[1 - parity],
        dst_ref=pair_in,
        send_sem=psend.at[0],
        recv_sem=precv.at[0],
        device_id={"sp": me + 1 - 2 * parity},
        device_id_type=MESH,
    )
    pairing.start()
    change = []
    key_part = []
    for b in range(blocks):
        rows = pl.ds(b * BLK, BLK)
        cumulative, middle, _ = decays(g_ref, rows)
        query = q_ref[rows, :].astype(jnp.float32) * scale
        key = k_ref[rows, :].astype(jnp.float32)
        value = v_ref[rows, :]
        d_out = d_ref[rows, :]
        rise, fall = jnp.exp(cumulative - middle), jnp.exp(middle - cumulative)
        lifted_q = (query * rise).astype(jnp.bfloat16)
        lifted_k = (key * fall).astype(jnp.bfloat16)
        scores = jnp.where(causal, mm(lifted_q, lifted_k, NT), 0.0).astype(jnp.bfloat16)
        d_scores = jnp.where(causal, mm(d_out, value, NT), 0.0).astype(jnp.bfloat16)
        d_lifted_q = mm(d_scores, lifted_k, NN)
        d_lifted_k = mm(d_scores, lifted_q, TN)
        grown = jnp.exp(cumulative)
        d_carried = mm(d_out, states_ref[b], NN) * grown
        gq_ref[rows, :] = ((d_lifted_q * rise + d_carried) * scale).astype(jnp.bfloat16)
        change.append(
            lifted_q.astype(jnp.float32) * d_lifted_q
            - lifted_k.astype(jnp.float32) * d_lifted_k
            + query * d_carried
        )
        key_part.append(d_lifted_k * fall)
        gg_ref[rows, :] = change[b]
        gv_ref[rows, :] = mm(scores, d_out, TN).astype(gv_ref.dtype)
    pairing.wait()
    for i in range(half):
        pair[i] = (part[parity, i].astype(jnp.float32) + pair_in[i].astype(jnp.float32)).astype(
            jnp.bfloat16
        )
    collect(n, me, -1, copies, recv, total, width)
    shares = []
    for s in range(1, half):
        other = lax.rem(mine + s, half)
        shares.append(
            pltpu.make_async_remote_copy(
                src_ref=pair.at[other],
                dst_ref=parts_in.at[s - 1],
                send_sem=psend.at[s],
                recv_sem=precv.at[s],
                device_id={"sp": 2 * other + parity},
                device_id_type=MESH,
            )
        )
        shares[-1].start()
    for b in range(blocks):
        rows = pl.ds(b * BLK, BLK)
        cumulative, _, ending = decays(g_ref, rows)
        d_state = kept[b] + total[...] * jnp.exp(afters[b])
        d_rounded = d_state.astype(jnp.bfloat16)
        key = k_ref[rows, :].astype(jnp.float32)
        fade = jnp.exp(ending - cumulative)
        faded = key * fade
        d_faded = mm(v_ref[rows, :], d_rounded, NN)
        gk_ref[rows, :] = (key_part[b] + d_faded * fade).astype(jnp.bfloat16)
        gv_ref[rows, :] = gv_ref[rows, :] + mm(faded.astype(jnp.bfloat16), d_rounded, NT)
        moved = faded * d_faded
        at_end = jnp.sum(moved, axis=0, keepdims=True) + jnp.exp(ending) * jnp.sum(
            states_ref[b].astype(jnp.float32) * d_state, axis=0, keepdims=True
        )
        gg_ref[rows, :] = block_sums(triangle(False), gg_ref[rows, :] - moved) + at_end
    summed = pair[mine].astype(jnp.float32)
    for s in range(1, half):
        shares[s - 1].wait()
        summed = summed + parts_in[s - 1].astype(jnp.float32)
    proj_ref[...] = summed


def exchange_scratch(n, blocks, width, channels):
    return [
        pltpu.VMEM((blocks, width, channels), jnp.float32),
        pltpu.VMEM((width, channels), jnp.float32),
        pltpu.VMEM((width + 16, channels), jnp.bfloat16),
        pltpu.VMEM((n - 1, width + 16, channels), jnp.bfloat16),
        pltpu.SemaphoreType.DMA((n - 1,)),
        pltpu.SemaphoreType.DMA((n - 1,)),
    ]


def in_vmem(count):
    return [pl.BlockSpec(memory_space=pltpu.VMEM)] * count


def mixer_forward(q, k, v, g, scale):
    n = lax.axis_size("sp")
    length, channels = q.shape
    width = v.shape[1]
    blocks = length // BLK
    return pl.pallas_call(
        functools.partial(forward_kernel, n, scale),
        out_shape=(
            jax.ShapeDtypeStruct((length, width), jnp.bfloat16),
            jax.ShapeDtypeStruct((blocks, width, channels), jnp.bfloat16),
        ),
        in_specs=in_vmem(4),
        out_specs=tuple(in_vmem(2)),
        scratch_shapes=exchange_scratch(n, blocks, width, channels),
        compiler_params=pltpu.CompilerParams(
            collective_id=1, has_side_effects=True, vmem_limit_bytes=16 * 1024 * 1024
        ),
        cost_estimate=pl.CostEstimate(
            flops=4_000_000_000, bytes_accessed=4 * length * width, transcendentals=0
        ),
        name="mixer_forward",
    )(q, k, v, g)


def mixer_backward(q, k, v, g, gathered, w_out, mixed, states, scale):
    n = lax.axis_size("sp")
    length, channels = q.shape
    width = v.shape[1]
    blocks = length // BLK
    share = w_out.shape[0] // n
    return pl.pallas_call(
        functools.partial(backward_kernel, n, scale),
        out_shape=(
            jax.ShapeDtypeStruct((length, channels), jnp.bfloat16),
            jax.ShapeDtypeStruct((length, channels), jnp.bfloat16),
            jax.ShapeDtypeStruct((length, width), jnp.float32),
            jax.ShapeDtypeStruct((length, channels), jnp.float32),
            jax.ShapeDtypeStruct((share, width), jnp.float32),
        ),
        in_specs=in_vmem(8),
        out_specs=tuple(in_vmem(5)),
        scratch_shapes=exchange_scratch(n, blocks, width, channels)
        + [
            pltpu.VMEM((length, width), jnp.bfloat16),
            pltpu.VMEM((2, n // 2, share, width), jnp.bfloat16),
            pltpu.VMEM((n // 2, share, width), jnp.bfloat16),
            pltpu.VMEM((n // 2, share, width), jnp.bfloat16),
            pltpu.VMEM((n // 2 - 1, share, width), jnp.bfloat16),
            pltpu.SemaphoreType.DMA((n // 2,)),
            pltpu.SemaphoreType.DMA((n // 2,)),
        ],
        compiler_params=pltpu.CompilerParams(
            collective_id=2, has_side_effects=True, vmem_limit_bytes=24 * 1024 * 1024
        ),
        cost_estimate=pl.CostEstimate(
            flops=8_000_000_000, bytes_accessed=4 * length * width, transcendentals=0
        ),
        name="mixer_backward",
    )(q, k, v, g, gathered, w_out, mixed, states)


def route_out(d_out, route_expert, route_weight, capacity):
    n, tp = lax.axis_size("sp"), lax.axis_size("tp")
    tokens, model_width = d_out.shape
    quarter = model_width // tp
    return pl.pallas_call(
        functools.partial(route_kernel, n, tp, capacity),
        out_shape=(
            jax.ShapeDtypeStruct((n, capacity, model_width), jnp.bfloat16),
            jax.ShapeDtypeStruct((2, tokens), jnp.int32),
        ),
        in_specs=in_vmem(3),
        out_specs=tuple(in_vmem(2)),
        scratch_shapes=[
            pltpu.VMEM((n, capacity, quarter), jnp.bfloat16),
            pltpu.SemaphoreType.DMA((n - 1,)),
            pltpu.SemaphoreType.DMA((n - 1,)),
            pltpu.SemaphoreType.DMA,
            pltpu.SemaphoreType.DMA((n, tp)),
            pltpu.SemaphoreType.DMA((n, tp)),
        ],
        compiler_params=pltpu.CompilerParams(
            collective_id=3, has_side_effects=True, vmem_limit_bytes=24 * 1024 * 1024
        ),
        cost_estimate=pl.CostEstimate(
            flops=8_000_000_000, bytes_accessed=4 * tokens * quarter, transcendentals=0
        ),
        name="route_out",
    )(d_out, route_expert.T, route_weight)


def route_back(summed, slots, d_out):
    n, tp = lax.axis_size("sp"), lax.axis_size("tp")
    capacity, quarter = summed.shape[1:]
    tokens = d_out.shape[0]
    return pl.pallas_call(
        functools.partial(return_kernel, n, tp, capacity),
        out_shape=jax.ShapeDtypeStruct((tp, tokens, quarter), jnp.bfloat16),
        in_specs=in_vmem(3),
        out_specs=in_vmem(1)[0],
        scratch_shapes=[
            pltpu.VMEM((n, capacity, quarter), jnp.bfloat16),
            pltpu.SemaphoreType.DMA((n - 1,)),
            pltpu.SemaphoreType.DMA((n - 1,)),
            pltpu.SemaphoreType.DMA,
            pltpu.SemaphoreType.DMA((tp,)),
            pltpu.SemaphoreType.DMA((tp,)),
        ],
        compiler_params=pltpu.CompilerParams(
            collective_id=4, has_side_effects=True, vmem_limit_bytes=24 * 1024 * 1024
        ),
        cost_estimate=pl.CostEstimate(
            flops=8_000_000_000, bytes_accessed=4 * tokens * quarter, transcendentals=0
        ),
        name="route_back",
    )(summed, slots, d_out)


def expert_pass(rows_in, routed_rows, gate_w, up_w, down_w):
    gate_pre = jnp.dot(rows_in, gate_w, preferred_element_type=jnp.float32)
    up_pre = jnp.dot(rows_in, up_w, preferred_element_type=jnp.float32)
    sigmoid_gate = jax.nn.sigmoid(gate_pre)
    active = gate_pre * sigmoid_gate
    hidden = (active * up_pre).astype(jnp.bfloat16)
    d_hidden = lax.dot_general(
        routed_rows, down_w, (((1,), (1,)), ((), ())), preferred_element_type=jnp.float32
    )
    d_gate = (d_hidden * up_pre * sigmoid_gate * (1.0 + gate_pre * (1.0 - sigmoid_gate))).astype(
        jnp.bfloat16
    )
    d_up = (d_hidden * active).astype(jnp.bfloat16)
    rows_first = (((0,), (0,)), ((), ()))
    grad_gate = lax.dot_general(
        rows_in, d_gate, rows_first, preferred_element_type=jnp.float32
    ).astype(jnp.bfloat16)
    grad_up = lax.dot_general(rows_in, d_up, rows_first, preferred_element_type=jnp.float32).astype(
        jnp.bfloat16
    )
    grad_down = lax.dot_general(
        hidden, routed_rows, rows_first, preferred_element_type=jnp.float32
    ).astype(jnp.bfloat16)
    return (grad_gate, grad_up, grad_down, d_gate, d_up)


def local(
    d_out,
    route_expert,
    route_weight,
    expert_inputs,
    w_gate,
    w_up,
    w_down,
    w_out,
    queries,
    keys,
    values,
    log_decay,
):
    model_width = d_out.shape[1]
    experts = lax.axis_size("sp")
    capacity = expert_inputs.shape[1] // experts
    quarter = model_width // lax.axis_size("tp")
    routed, slots = route_out(d_out, route_expert, route_weight, capacity)
    routed = routed.reshape(experts * capacity, model_width)
    rows_in = expert_inputs[0]
    gate_w = w_gate[0]
    up_w = w_up[0]
    grad_gate, grad_up, grad_down, d_gate, d_up = expert_pass(
        rows_in, routed, gate_w, up_w, w_down[0]
    )
    partial_terms = lax.dot_general(
        d_gate, gate_w, (((1,), (1,)), ((), ())), preferred_element_type=jnp.float32
    )
    partial_terms = partial_terms + lax.dot_general(
        d_up, up_w, (((1,), (1,)), ((), ())), preferred_element_type=jnp.float32
    )
    rounded = lax.optimization_barrier(partial_terms.astype(jnp.bfloat16)).astype(jnp.float32)
    summed = lax.psum_scatter(rounded.astype(jnp.bfloat16), "tp", scatter_dimension=1, tiled=True)
    scale_q = queries.shape[2] ** (-0.5)
    q, k, v, g = queries[:, 0], keys[:, 0], values[:, 0], log_decay[:, 0]
    mixed, states = mixer_forward(q, k, v, g, scale_q)
    summed, mixed, grad_gate, grad_up, grad_down = lax.optimization_barrier(
        (summed, mixed, grad_gate, grad_up, grad_down)
    )
    gathered = route_back(summed.reshape(experts, capacity, quarter), slots, d_out)
    grad_q, grad_k, grad_v, grad_g, grad_proj = mixer_backward(
        q, k, v, g, gathered, w_out, mixed, states, scale_q
    )
    return (
        grad_gate[None],
        grad_up[None],
        grad_down[None],
        grad_proj,
        grad_q[:, None],
        grad_k[:, None],
        grad_v.astype(jnp.bfloat16)[:, None],
        grad_g[:, None],
    )


def solution(mesh):
    return jax.shard_map(
        local,
        mesh=mesh,
        in_specs=(
            P("sp", None),
            P("sp", None),
            P("sp", None),
            P("sp", None, None),
            P("sp", None, "tp"),
            P("sp", None, "tp"),
            P("sp", "tp", None),
            P(None, "tp"),
            P("sp", "tp", None),
            P("sp", "tp", None),
            P("sp", "tp", None),
            P("sp", "tp", None),
        ),
        out_specs=(
            P("sp", None, "tp"),
            P("sp", None, "tp"),
            P("sp", "tp", None),
            P("sp", "tp"),
            P("sp", "tp", None),
            P("sp", "tp", None),
            P("sp", "tp", None),
            P("sp", "tp", None),
        ),
        check_vma=False,
    )
```
